32 devices in a mesh: sp: 8 (over z, y), tp: 4 (over x, core).
Axes of the slice: x: 2, y: 2, z: 4, core: 2. Of those that a mesh axis runs over, the one named last changes fastest.
Arguments:
- stream: bfloat16 [2048, 2048], P('sp'), may hold values from -6 to 6
- pooled_in: bfloat16 [2048, 1024], P('sp', 'tp'), may hold values from -6 to 6
- pool_weight: bfloat16 [4, 256, 256], P('tp'), may hold values from -0.375 to 0.375
- pool_scale: float32 [1024], P('tp'), may hold values from 0.1 to 1.9
- out_weight: bfloat16 [1024, 2048], replicated, may hold values from -0.1875 to 0.1875
- norm_gain: float32 [2048], replicated, may hold values from 0.1 to 1.9
- routes: int32 [2048, 3], P('sp'), may hold values from 0 to 7, all different within a row; in each aligned block of 64 rows (0 to 63, 64 to 127, ...) at most 48 rows name the same one
- route_weights: float32 [2048, 3], P('sp'), may hold values from 0.25 to 2.5
- expert_gate: bfloat16 [8, 2048, 2048], P('sp', None, 'tp'), may hold values from -0.125 to 0.125
- expert_up: bfloat16 [8, 2048, 2048], P('sp', None, 'tp'), may hold values from -0.125 to 0.125
- expert_down: bfloat16 [8, 2048, 2048], P('sp', 'tp'), may hold values from -0.125 to 0.125
- shared_gate: bfloat16 [2048, 512], P(None, 'tp'), may hold values from -0.125 to 0.125
- shared_up: bfloat16 [2048, 512], P(None, 'tp'), may hold values from -0.125 to 0.125
- shared_down: bfloat16 [512, 2048], P('tp'), may hold values from -0.25 to 0.25
Outputs:
- layer_out: bfloat16 [2048, 2048], P(('sp', 'tp'))
The draws below stay inside these ranges and needn't reach their ends.
Inputs may be any that keep to these rules, and one draw needn't show every extreme that they name: `routes`: each row names 3 different experts. In each aligned block of 64 rows (the rows of one device in the layer's output) no expert is named by more than 48 rows, a bound that some block reaches.
All inputs are finite; a program needn't handle non-finite values.
Results may differ from the reference program's by a relative error of at most 0.012.
Values may be sent and summed in bfloat16 or wider, within the bound.
A program may use at most 128 MiB of HBM per device.

```python
import math
import jax
import jax.numpy as jnp
import numpy as np
from jax import lax

D = 2048
WINDOWS = 4
PW = 1024
PG = 256
REACH = 16
EFF = 2048
SFF = 512
TOPK = 3
TOKENS = 2048
ROWS_DEV = 64
EXPERTS = 8
CAP = 48
N_SP = 8
N_TP = 4


def shard_levels(own_key, dims, pieces, least, top_value):
    loudness, own = 1.0, jax.random.fold_in(own_key, 6)
    for dim, shards_of in pieces:
        heights = jnp.exp(jax.random.uniform(jax.random.fold_in(own, dim), (shards_of,), jnp.float32, least / len(pieces), top_value / len(pieces)))
        loudness = loudness * jnp.repeat(heights, dims[dim] // shards_of).reshape([-1 if axis == dim else 1 for axis in range(len(dims))])
    return loudness


def assign_block(own_key, own, number, rows, amount, top, most, lean):
    sequence = jax.random.permutation(own_key, amount)
    crowded, usual = shares(amount, rows * top, most, lean, True), shares(amount, rows * top, most, lean, False)
    places = jnp.arange(amount)

    def named(tallies, rotation):
        used = int((tallies > 0).sum())
        fixed = max(1, used // 4)
        moved = fixed + (places - fixed + rotation * (used - fixed)) % max(1, amount - fixed)
        return jnp.zeros((amount,), jnp.int32).at[sequence[jnp.where(places < fixed, places, moved)]].set(jnp.asarray(tallies, jnp.int32))

    tallies = jnp.where(number % 4 == 0, named(crowded, number // 4), named(usual, number - number // 4 - 1))
    mixed = jax.random.permutation(jax.random.fold_in(own, 3), amount)
    source_of, sink = mixed[0:amount // 2 * 2:2], mixed[1:amount // 2 * 2:2]
    slack = jnp.minimum(tallies[source_of] - 1, most - tallies[sink]) // 2
    slack = jnp.where((source_of == sequence[0]) | (sink == sequence[0]) | (tallies[sink] == 0), 0, jnp.maximum(slack, 0))
    moved = jax.random.randint(jax.random.fold_in(own, 4), (amount // 2,), 0, 1 << 20) % (slack + 1)
    tallies = tallies.at[source_of].add(-moved).at[sink].add(moved)
    items = jnp.searchsorted(jnp.cumsum(tallies), jnp.arange(rows * top), side="right").astype(jnp.int32)
    table = items.reshape(top, rows).T
    table = table[jax.random.permutation(jax.random.fold_in(own, 1), rows)]
    rotation = jax.random.randint(jax.random.fold_in(own, 2), (rows, 1), 0, top)
    return jnp.take_along_axis(table, (jnp.arange(top)[None, :] + rotation) % top, axis=1)


def shares(count, total, most, skew, full):
    loads = [(1 << 20) // math.isqrt(rank ** skew) + 1 for rank in range(1, count + 1)]
    largest = most if full else min(most, max(-(-total // count), total * loads[0] // sum(loads)))
    least = 1 if total - largest >= count - 1 else 0
    holding, spare = [largest] + [least] * (count - 1), total - largest - least * (count - 1)
    while spare > 0:
        candidates = [i for i in range(1, count) if holding[i] < largest] or [i for i in range(1, count) if holding[i] < most]
        mass, budget = sum([loads[i] for i in candidates]), spare
        for i in candidates:
            more = min(most - holding[i], max(1, budget * loads[i] // mass), spare)
            holding[i] = holding[i] + more
            spare = spare - more
    return np.array(holding)


def noise(key, dims, scale, bound, pieces=(), held_as=jnp.bfloat16):
    entries = scale * jax.random.normal(key, dims, jnp.float32)
    if pieces:
        entries = entries * shard_levels(key, dims, pieces, -0.22, 0.18)
    return jnp.clip(entries, -bound, bound).astype(held_as)


def setup_inputs(seed: int = 0) -> dict:
    splits = jax.random.split(jax.random.key(seed), 15)
    stream = noise(splits[0], (TOKENS, D), 1.0, 6.0, ((0, 8),))
    pooled_in = noise(splits[1], (TOKENS, PW), 1.0, 6.0, ((0, 8), (1, 4)))
    pool_weight = noise(splits[2], (WINDOWS, PG, PG), PG ** -0.5, 0.375, ((0, 4),))
    pool_scale = jnp.clip(1.0 + 0.18 * jax.random.normal(splits[3], (PW,), jnp.float32), 0.1, 1.9)
    out_weight = noise(splits[4], (PW, D), PW ** -0.5, 0.1875)
    norm_gain = jnp.clip(1.0 + 0.18 * jax.random.normal(splits[5], (D,), jnp.float32), 0.1, 1.9)
    routes_keys = jax.random.split(jax.random.fold_in(splits[6], 1), TOKENS // ROWS_DEV)
    routes_turns = jax.random.permutation(jax.random.fold_in(splits[6], 3), TOKENS // ROWS_DEV)
    routes = jax.vmap(lambda own, number: assign_block(jax.random.fold_in(splits[6], 2), own, number, ROWS_DEV, EXPERTS, TOPK, CAP, 1))(routes_keys, routes_turns).reshape((TOKENS, TOPK))
    route_weights = jnp.clip(jnp.exp(math.log(2.5) - 2.3025851 * jax.random.uniform(splits[7], (TOKENS, TOPK), jnp.float32) ** shard_levels(splits[7], (TOKENS, TOPK), ((0, 8),), -0.2, 0.2)), 0.25, 2.5)
    expert_gate = noise(splits[8], (EXPERTS, D, EFF), D ** -0.5, 0.125, ((0, 8), (2, 4)))
    expert_up = noise(splits[9], (EXPERTS, D, EFF), D ** -0.5, 0.125, ((0, 8), (2, 4)))
    expert_down = noise(splits[10], (EXPERTS, EFF, D), EFF ** -0.5, 0.125, ((0, 8), (1, 4)))
    shared_gate = noise(splits[11], (D, SFF), D ** -0.5, 0.125, ((1, 4),))
    shared_up = noise(splits[12], (D, SFF), D ** -0.5, 0.125, ((1, 4),))
    shared_down = noise(splits[13], (SFF, D), SFF ** -0.5, 0.25, ((0, 4),))
    return {"stream": stream, "pooled_in": pooled_in, "pool_weight": pool_weight, "pool_scale": pool_scale, "out_weight": out_weight, "norm_gain": norm_gain, "routes": routes, "route_weights": route_weights, "expert_gate": expert_gate, "expert_up": expert_up, "expert_down": expert_down, "shared_gate": shared_gate, "shared_up": shared_up, "shared_down": shared_down}


EPSILON = 1e-06

def down_rounded(hidden, weight):
    group_rows = weight.shape[0] // N_TP
    summed = jnp.zeros((hidden.shape[0], weight.shape[1]), jnp.float32)
    for part_index in range(N_TP):
        partial_value = jnp.dot(hidden[:, part_index * group_rows:(part_index + 1) * group_rows], weight[part_index * group_rows:(part_index + 1) * group_rows], preferred_element_type=jnp.float32)
        summed = summed + lax.optimization_barrier(partial_value.astype(jnp.bfloat16)).astype(jnp.float32)
    return summed

def reference(stream, pooled_in, pool_weight, pool_scale, out_weight, norm_gain, routes, route_weights, expert_gate, expert_up, expert_down, shared_gate, shared_up, shared_down):
    tokens_all = stream.shape[0]
    position = jnp.arange(tokens_all, dtype=jnp.int32)
    group_outs = []
    for group_index in range(WINDOWS):
        window = 2 ** (group_index + 1)
        channels = pooled_in[:, group_index * PG:(group_index + 1) * PG].astype(jnp.float32)
        padded = jnp.concatenate([jnp.zeros((REACH - 1, PG), jnp.float32), channels], 0)
        summed = jnp.zeros_like(channels)
        for lag_step in range(window):
            summed = summed + padded[REACH - 1 - lag_step:REACH - 1 - lag_step + tokens_all]
        counted = jnp.minimum(position + 1, window).astype(jnp.float32)
        pooled = (summed / counted[:, None] - channels).astype(jnp.bfloat16)
        mixed_group = jnp.dot(pooled, pool_weight[group_index], preferred_element_type=jnp.float32)
        mixed_group = mixed_group * pool_scale[group_index * PG:(group_index + 1) * PG]
        group_outs.append(mixed_group.astype(jnp.bfloat16))
    grouped = jnp.concatenate(group_outs, 1)
    mixed_all = jnp.dot(grouped, out_weight, preferred_element_type=jnp.float32)
    residual = (stream.astype(jnp.float32) + mixed_all).astype(jnp.bfloat16)
    resid_wide = residual.astype(jnp.float32)
    normed = (resid_wide * lax.rsqrt(lax.optimization_barrier(jnp.mean(resid_wide * resid_wide, axis=-1, keepdims=True)) + EPSILON) * norm_gain).astype(jnp.bfloat16)
    most_rows = N_SP * N_TP * CAP
    slot_iota = jnp.arange(most_rows, dtype=jnp.int32)
    expert_ids = jnp.arange(EXPERTS, dtype=jnp.int32)

    def one_expert(running, inputs):
        w_gate, w_up, w_down, expert_id = inputs
        chosen = routes == expert_id
        member = jnp.any(chosen, axis=1)
        weight = lax.optimization_barrier(jnp.sum(jnp.where(chosen, route_weights, jnp.zeros_like(route_weights)), axis=1))
        picked = jnp.nonzero(member, size=most_rows, fill_value=0)[0].astype(jnp.int32)
        valid_rows = (slot_iota < jnp.sum(member.astype(jnp.int32))).astype(jnp.float32)
        row_data = normed[picked]
        hidden = (jax.nn.silu(jnp.dot(row_data, w_gate, preferred_element_type=jnp.float32)) * jnp.dot(row_data, w_up, preferred_element_type=jnp.float32)).astype(jnp.bfloat16)
        result = lax.optimization_barrier(down_rounded(hidden, w_down).astype(jnp.bfloat16)).astype(jnp.float32)
        scaled = result * (weight[picked] * valid_rows)[:, None]
        return (running.at[picked].add(scaled), None)
    routed, _ = lax.scan(one_expert, jnp.zeros((tokens_all, D), jnp.float32), (expert_gate, expert_up, expert_down, expert_ids))
    shared_hidden = (jax.nn.silu(jnp.dot(normed, shared_gate, preferred_element_type=jnp.float32)) * jnp.dot(normed, shared_up, preferred_element_type=jnp.float32)).astype(jnp.bfloat16)
    shared = down_rounded(shared_hidden, shared_down)
    return (residual.astype(jnp.float32) + routed + shared).astype(jnp.bfloat16)
```

```python
import functools
import jax
import jax.numpy as jnp
from jax import lax
from jax.experimental import pallas as pl
from jax.experimental.pallas import tpu as pltpu
from jax.sharding import PartitionSpec as P

REACH = 16


EPSILON = 1e-06
WINDOW_GROUPS = 4


def passed_along(value, axis, steps):
    count = lax.axis_size(axis)
    initial, last = (max(0, -steps), min(count, count - steps))
    return lax.ppermute(value, axis, [(source, source + steps) for source in range(initial, last)])


def slot_positions(route_block, n_experts, capacity):
    flat_ids = route_block.reshape(-1)
    onehot = (flat_ids[:, None] == jnp.arange(n_experts, dtype=jnp.int32)[None, :]).astype(
        jnp.int32
    )
    earlier = jnp.cumsum(onehot, axis=0) - onehot
    rank_in = jnp.sum(earlier * onehot, axis=1)
    return flat_ids * capacity + rank_in


def on_device(
    stream,
    pooled_in,
    pool_weight,
    pool_scale,
    out_weight,
    norm_gain,
    routes,
    route_weights,
    expert_gate,
    expert_up,
    expert_down,
    shared_gate,
    shared_up,
    shared_down,
):
    tok_dev, group_width = pooled_in.shape
    model_width = stream.shape[1]
    tp_size = lax.axis_size("tp")
    sp_size = lax.axis_size("sp")
    tp_index = lax.axis_index("tp")
    sp_index = lax.axis_index("sp")
    top_count = routes.shape[1]
    rows_dev = tok_dev // tp_size
    capacity = max(2, 2 * rows_dev * top_count // sp_size)
    window = lax.shift_left(jnp.int32(2), tp_index)
    rim_rows = passed_along(pooled_in[tok_dev - (REACH - 1) :], "sp", 1)
    padded = jnp.concatenate([rim_rows, pooled_in], 0).astype(jnp.float32)
    summed = jnp.zeros((tok_dev, group_width), jnp.float32)
    for lag_step in range(REACH):
        enabled = (lag_step < window).astype(jnp.float32)
        summed = summed + padded[REACH - 1 - lag_step : REACH - 1 - lag_step + tok_dev] * enabled
    position = sp_index * tok_dev + jnp.arange(tok_dev, dtype=jnp.int32)
    counted = jnp.minimum(position + 1, window).astype(jnp.float32)
    pooled = (summed / counted[:, None] - padded[REACH - 1 :]).astype(jnp.bfloat16)
    group_mix = (
        jnp.dot(pooled, pool_weight[0], preferred_element_type=jnp.float32) * pool_scale
    ).astype(jnp.bfloat16)
    mixed_all = jnp.dot(
        lax.all_gather(group_mix, "tp", axis=1, tiled=True),
        out_weight,
        preferred_element_type=jnp.float32,
    )
    residual = (stream.astype(jnp.float32) + mixed_all).astype(jnp.bfloat16)
    resid_wide = residual.astype(jnp.float32)
    normed = (
        resid_wide
        * lax.rsqrt(jnp.mean(resid_wide * resid_wide, axis=-1, keepdims=True) + EPSILON)
        * norm_gain
    ).astype(jnp.bfloat16)
    own_begin = tp_index * rows_dev
    own_routes = lax.dynamic_slice_in_dim(routes, own_begin, rows_dev, 0)
    own_pos = slot_positions(own_routes, sp_size, capacity)
    own_normed = lax.dynamic_slice_in_dim(normed, own_begin, rows_dev, 0)
    sending = jnp.zeros((sp_size * capacity, model_width), jnp.bfloat16)
    sending = sending.at[own_pos].set(jnp.repeat(own_normed, top_count, axis=0))
    landed = lax.all_to_all(
        sending.reshape(sp_size, capacity, model_width),
        "sp",
        split_axis=0,
        concat_axis=0,
        tiled=True,
    )
    arrived = lax.all_gather(landed[None], "tp", axis=0, tiled=True)
    arrived = arrived.reshape(-1, model_width)
    rows_in = arrived
    hidden = (
        jax.nn.silu(jnp.dot(rows_in, expert_gate[0], preferred_element_type=jnp.float32))
        * jnp.dot(rows_in, expert_up[0], preferred_element_type=jnp.float32)
    ).astype(jnp.bfloat16)
    expert_out = lax.psum_scatter(
        jnp.dot(hidden, expert_down[0], preferred_element_type=jnp.float32).astype(jnp.bfloat16),
        "tp",
        scatter_dimension=0,
        tiled=True,
    )
    returned = lax.all_to_all(
        expert_out.reshape(sp_size, capacity, model_width),
        "sp",
        split_axis=0,
        concat_axis=0,
        tiled=True,
    )
    picked = jnp.take(returned.reshape(-1, model_width), own_pos, axis=0)
    picked = picked.reshape(rows_dev, top_count, model_width)
    own_weights = lax.dynamic_slice_in_dim(route_weights, own_begin, rows_dev, 0)
    routed = jnp.sum(picked.astype(jnp.float32) * own_weights[:, :, None], axis=1)
    rows_in = normed
    hidden = (
        jax.nn.silu(jnp.dot(rows_in, shared_gate, preferred_element_type=jnp.float32))
        * jnp.dot(rows_in, shared_up, preferred_element_type=jnp.float32)
    ).astype(jnp.bfloat16)
    shared = lax.psum_scatter(
        jnp.dot(hidden, shared_down, preferred_element_type=jnp.float32).astype(jnp.bfloat16),
        "tp",
        scatter_dimension=0,
        tiled=True,
    ).astype(jnp.float32)
    own_resid = lax.dynamic_slice_in_dim(residual, own_begin, rows_dev, 0).astype(jnp.float32)
    return (own_resid + routed + shared).astype(jnp.bfloat16)


VMEM_ROOM = 40 * 2**20
LANES = 128


def exchange_kernel(
    nz,
    rows,
    width,
    packed_ref,
    resid_ref,
    gate_hbm,
    up_hbm,
    down_hbm,
    sgate_hbm,
    sup_hbm,
    sdown_hbm,
    out_ref,
    gbuf,
    acc,
    pbuf,
    rcbuf,
    sbuf_b,
    rbuf_b,
    sbuf_a,
    rbuf_a,
    sbuf_z,
    rbuf_z,
    hid,
    shid,
    wgate,
    wup,
    wdown,
    wsgate,
    wsup,
    wsdown,
    wsem,
    osem,
    zs,
    zr,
    a_s,
    a_r,
    bs,
    br,
    cs,
    cr,
    rcs,
    rcr,
    rbs,
    rbr,
    ras,
    rar,
    rzs,
    rzr,
):
    sp = lax.axis_index("sp")
    tp = lax.axis_index("tp")
    z, y = sp // 2, sp % 2
    x, c = tp // 2, tp % 2

    def dev(zz, yy, xx, cc):
        return (zz * 2 + yy, xx * 2 + cc)

    peer_a = dev(z, y + (1 - c) * (1 - 2 * y), x + c * (1 - 2 * x), c)
    peer_b = dev(z, y + c * (1 - 2 * y), x + (1 - c) * (1 - 2 * x), c)
    peer_c = dev(z, y, x, 1 - c)

    def peer_z(k):
        return dev((z + k) % nz, y, x, c)

    def rdma(src, dst, ssem, rsem, device):
        return pltpu.make_async_remote_copy(
            src_ref=src,
            dst_ref=dst,
            send_sem=ssem,
            recv_sem=rsem,
            device_id=device,
            device_id_type=pl.DeviceIdType.MESH,
        )

    def blk(cls, d, j):
        return gbuf.at[cls, d, pl.ds(j * rows, rows)]

    weight_pairs = (
        (gate_hbm.at[0], wgate),
        (up_hbm.at[0], wup),
        (down_hbm.at[0], wdown),
        (sgate_hbm, wsgate),
        (sup_hbm, wsup),
        (sdown_hbm, wsdown),
    )
    weight_copies = [
        pltpu.make_async_copy(s, t, wsem.at[i]) for i, (s, t) in enumerate(weight_pairs)
    ]
    own_copy = pltpu.make_async_copy(packed_ref, blk(0, 0, 0), osem)
    own_copy.start()
    for copy in weight_copies:
        copy.start()

    barrier = pltpu.get_barrier_semaphore()
    peers = [peer_z(k) for k in range(1, nz)] + [peer_a, peer_b, peer_c]
    for peer in peers:
        pl.semaphore_signal(
            barrier, inc=1, device_id=peer, device_id_type=pl.DeviceIdType.MESH
        )
    pl.semaphore_wait(barrier, len(peers))
    own_copy.wait()

    def z_copy(k):
        return rdma(blk(0, 0, 0), blk(0, nz - k, 0), zs.at[k], zr.at[nz - k], peer_z(k))

    def z_recv(d):
        return rdma(blk(0, 0, 0), blk(0, d, 0), zs.at[d], zr.at[d], peer_z(d))

    def a_copy(d):
        return rdma(blk(0, d, 0), blk(0, d, 1), a_s.at[d], a_r.at[d], peer_a)

    def b_copy(d, a):
        return rdma(blk(0, d, a), blk(0, d, 2 + a), bs.at[2 * d + a], br.at[2 * d + a], peer_b)

    def c_copy(d, j):
        return rdma(blk(0, d, j), blk(1, d, j), cs.at[4 * d + j], cr.at[4 * d + j], peer_c)

    def first_pass(d):
        a_copy(d).start()
        b_copy(d, 0).start()
        c_copy(d, 0).start()

    def second_pass(d):
        a_copy(d).wait_recv()
        b_copy(d, 1).start()
        c_copy(d, 1).start()

    def rc_copy(d):
        return rdma(pbuf.at[d], rcbuf.at[d], rcs.at[d], rcr.at[d], peer_c)

    def rb_copy(d):
        return rdma(sbuf_b.at[d], rbuf_b.at[d], rbs.at[d], rbr.at[d], peer_b)

    def ra_copy(d):
        return rdma(sbuf_a.at[d], rbuf_a.at[d], ras.at[d], rar.at[d], peer_a)

    def rz_copy(d):
        return rdma(sbuf_z.at[d], rbuf_z.at[nz - d], rzs.at[d], rzr.at[nz - d], peer_z(d))

    def rz_recv(d):
        return rdma(sbuf_z.at[d], rbuf_z.at[d], rzs.at[d], rzr.at[d], peer_z(d))

    dot = functools.partial(jnp.dot, preferred_element_type=jnp.float32)
    step_in = min(256, wgate.shape[1])
    step_out = min(512, width)

    def hidden_of(cls, d, gate, up, result, step):
        @pl.loop(0, gate.shape[1] // step)
        def _(i):
            cols = pl.ds(pl.multiple_of(i * step, step), step)
            block = gbuf[cls, d, :, 0:width]
            g = dot(block, gate[:, cols])
            u = dot(block, up[:, cols])
            result[:, cols] = (g / (1.0 + jnp.exp(-g)) * u).astype(jnp.bfloat16)

    def expert(cls, d, store):
        hidden_of(cls, d, wgate, wup, hid, step_in)
        tags = gbuf[cls, d, :, width : width + LANES].astype(jnp.float32)
        lane = lax.broadcasted_iota(jnp.int32, tags.shape, 1)
        mine = (lane == sp) | (lane == sp + LANES // 2)
        weight = jnp.sum(jnp.where(mine, tags, 0.0), axis=1, keepdims=True)

        @pl.when(d > 0)
        def _():
            @pl.loop(0, width // step_out)
            def _(i):
                cols = pl.ds(pl.multiple_of(i * step_out, step_out), step_out)
                store(cols, dot(hid[...], wdown[:, cols]) * weight)

        @pl.when(d == 0)
        def _():
            hidden_of(cls, d, wsgate, wsup, shid, wsgate.shape[1])
            group = lax.broadcasted_iota(jnp.int32, weight.shape, 0) // rows
            flag = jnp.where((c + cls) % 2 == 0, group % 2, group // 2)
            near = jnp.where(flag == 0, 1.0, 0.0)

            @pl.loop(0, width // step_out)
            def _(i):
                cols = pl.ds(pl.multiple_of(i * step_out, step_out), step_out)
                store(
                    cols,
                    dot(hid[...], wdown[:, cols]) * weight
                    + dot(shid[...], wsdown[:, cols]) * near,
                )

    def wide(value):
        return value.astype(jnp.float32)

    def reduce_b(d):
        rc_copy(d).wait_recv()
        upper = pl.ds(2 * rows, 2 * rows)
        sbuf_b[d] = (acc[d, upper, :] + wide(rcbuf[d, upper, :])).astype(jnp.bfloat16)
        rb_copy(d).start()

    def reduce_a(d):
        rb_copy(d).wait_recv()
        part = pl.ds(rows, rows)
        total = acc[d, part, :] + wide(rcbuf[d, part, :]) + wide(rbuf_b[d, part, :])
        sbuf_a[d] = total.astype(jnp.bfloat16)
        ra_copy(d).start()

    def base_total(d):
        part = pl.ds(0, rows)
        return (
            acc[d, part, :]
            + wide(rcbuf[d, part, :])
            + wide(rbuf_b[d, part, :])
            + wide(rbuf_a[d])
        )

    def reduce_z(d):
        ra_copy(d).wait_recv()

        @pl.when(d > 0)
        def _():
            sbuf_z[d] = base_total(d).astype(jnp.bfloat16)
            rz_copy(d).start()

    for k in range(1, nz):
        z_copy(k).start()
    first_pass(0)
    second_pass(0)
    for copy in weight_copies:
        copy.wait()

    @pl.loop(0, nz)
    def _(d):
        @pl.when(d < nz - 1)
        def _():
            z_recv(d + 1).wait_recv()
            first_pass(d + 1)

        for a in range(2):
            b_copy(d, a).wait_recv()
            c_copy(d, 2 + a).start()

        def store_acc(cols, value):
            acc[d, :, cols] = value

        expert(0, d, store_acc)

        @pl.when(d < nz - 1)
        def _():
            second_pass(d + 1)

        for j in range(4):
            c_copy(d, j).wait_recv()

        def store_part(cols, value):
            pbuf[d, :, cols] = value.astype(jnp.bfloat16)

        expert(1, d, store_part)
        rc_copy(d).start()
        reduce_b(d)

        @pl.when(d >= 1)
        def _():
            reduce_a(d - 1)

        @pl.when(d >= 2)
        def _():
            reduce_z(d - 2)

    reduce_a(nz - 1)
    reduce_z(nz - 2)
    reduce_z(nz - 1)
    total = base_total(0) + wide(resid_ref[...])
    for d in range(1, nz):
        rz_recv(d).wait_recv()
        total = total + wide(rbuf_z[d])
    out_ref[...] = total.astype(jnp.bfloat16)

    for k in range(1, nz):
        z_copy(k).wait_send()
        rz_copy(k).wait_send()

    @pl.loop(0, nz)
    def _(d):
        a_copy(d).wait_send()
        for a in range(2):
            b_copy(d, a).wait_send()
        for j in range(4):
            c_copy(d, j).wait_send()
        rc_copy(d).wait_send()
        rb_copy(d).wait_send()
        ra_copy(d).wait_send()


def exchanged(packed, resid, weights, nz):
    rows, width = resid.shape
    gate, up, down, sgate, sup, sdown = weights
    bf16, f32 = jnp.bfloat16, jnp.float32
    four, two = 4 * rows, 2 * rows
    vm = pltpu.VMEM
    dma = pltpu.SemaphoreType.DMA
    any_spec = pl.BlockSpec(memory_space=pl.ANY)
    vmem_spec = pl.BlockSpec(memory_space=pltpu.VMEM)
    return pl.pallas_call(
        functools.partial(exchange_kernel, nz, rows, width),
        out_shape=jax.ShapeDtypeStruct((rows, width), bf16),
        in_specs=[vmem_spec] * 2 + [any_spec] * 6,
        out_specs=vmem_spec,
        scratch_shapes=[
            vm((2, nz, four, width + LANES), bf16),
            vm((nz, four, width), f32),
            vm((nz, four, width), bf16),
            vm((nz, four, width), bf16),
            vm((nz, two, width), bf16),
            vm((nz, two, width), bf16),
            vm((nz, rows, width), bf16),
            vm((nz, rows, width), bf16),
            vm((nz, rows, width), bf16),
            vm((nz, rows, width), bf16),
            vm((four, gate.shape[2]), bf16),
            vm((four, sgate.shape[1]), bf16),
            vm(gate.shape[1:], bf16),
            vm(up.shape[1:], bf16),
            vm(down.shape[1:], bf16),
            vm(sgate.shape, bf16),
            vm(sup.shape, bf16),
            vm(sdown.shape, bf16),
            dma((6,)),
            dma,
        ]
        + [dma((n,)) for n in (nz, nz, nz, nz, 2 * nz, 2 * nz, 4 * nz, 4 * nz)]
        + [dma((nz,)) for _ in range(8)],
        compiler_params=pltpu.CompilerParams(
            collective_id=0, has_side_effects=True, vmem_limit_bytes=60 * 2**20
        ),
        name="exchange_experts",
    )(packed, resid, gate, up, down, sgate, sup, sdown)


def on_device_dense(
    stream,
    pooled_in,
    pool_weight,
    pool_scale,
    out_weight,
    norm_gain,
    routes,
    route_weights,
    expert_gate,
    expert_up,
    expert_down,
    shared_gate,
    shared_up,
    shared_down,
):
    tok_dev, group_width = pooled_in.shape
    tp_size = lax.axis_size("tp")
    sp_size = lax.axis_size("sp")
    tp_index = lax.axis_index("tp")
    sp_index = lax.axis_index("sp")
    rows_dev = tok_dev // tp_size
    window = lax.shift_left(jnp.int32(2), tp_index)
    rim_rows = passed_along(pooled_in[tok_dev - (REACH - 1) :], "sp", 1)
    padded = jnp.concatenate([rim_rows, pooled_in], 0).astype(jnp.float32)
    summed = jnp.zeros((tok_dev, group_width), jnp.float32)
    for lag_step in range(REACH):
        enabled = (lag_step < window).astype(jnp.float32)
        summed = summed + padded[REACH - 1 - lag_step : REACH - 1 - lag_step + tok_dev] * enabled
    position = sp_index * tok_dev + jnp.arange(tok_dev, dtype=jnp.int32)
    counted = jnp.minimum(position + 1, window).astype(jnp.float32)
    pooled = (summed / counted[:, None] - padded[REACH - 1 :]).astype(jnp.bfloat16)
    group_mix = (
        jnp.dot(pooled, pool_weight[0], preferred_element_type=jnp.float32) * pool_scale
    ).astype(jnp.bfloat16)
    own_begin = tp_index * rows_dev
    own_mix = lax.all_to_all(group_mix, "tp", split_axis=0, concat_axis=1, tiled=True)
    mixed_all = jnp.dot(own_mix, out_weight, preferred_element_type=jnp.float32)
    own_stream = lax.dynamic_slice_in_dim(stream, own_begin, rows_dev, 0)
    residual = (own_stream.astype(jnp.float32) + mixed_all).astype(jnp.bfloat16)
    resid_wide = residual.astype(jnp.float32)
    normed = (
        resid_wide
        * lax.rsqrt(jnp.mean(resid_wide * resid_wide, axis=-1, keepdims=True) + EPSILON)
        * norm_gain
    ).astype(jnp.bfloat16)
    own_routes = lax.dynamic_slice_in_dim(routes, own_begin, rows_dev, 0)
    own_weights = lax.dynamic_slice_in_dim(route_weights, own_begin, rows_dev, 0)
    ids = jnp.arange(LANES // 2, dtype=jnp.int32)
    table = jnp.sum(
        jnp.where(own_routes[:, :, None] == ids, own_weights[:, :, None], 0.0), axis=1
    )
    high = lax.reduce_precision(table, 8, 7)
    tags = jnp.concatenate([high, table - high], 1).astype(jnp.bfloat16)
    packed = jnp.concatenate([normed, tags], 1)
    weights = (expert_gate, expert_up, expert_down, shared_gate, shared_up, shared_down)
    return exchanged(packed, residual, weights, sp_size // 2)


def held_whole(mesh, *args):
    stream, expert_gate = args[0], args[8]
    sp_size, tp_size = mesh.shape["sp"], mesh.shape["tp"]
    return (
        3 * stream.size * stream.dtype.itemsize <= VMEM_ROOM
        and sp_size % 2 == 0
        and sp_size <= LANES // 2
        and tp_size == WINDOW_GROUPS
        and expert_gate.shape[0] == sp_size
    )


def solution(mesh):
    placed = (
        P("sp", None),
        P("sp", "tp"),
        P("tp", None, None),
        P("tp"),
        P(),
        P(),
        P("sp", None),
        P("sp", None),
        P("sp", None, "tp"),
        P("sp", None, "tp"),
        P("sp", "tp", None),
        P(None, "tp"),
        P(None, "tp"),
        P("tp", None),
    )

    def layer(*args):
        body = on_device_dense if held_whole(mesh, *args) else on_device
        return jax.shard_map(
            body, mesh=mesh, in_specs=placed, out_specs=P(("sp", "tp"), None), check_vma=False
        )(*args)

    return layer
```

```python
import functools
import jax
import jax.numpy as jnp
from jax import lax
from jax.experimental import pallas as pl
from jax.experimental.pallas import tpu as pltpu
from jax.sharding import PartitionSpec as P

REACH = 16


EPSILON = 1e-06
WINDOW_GROUPS = 4


def passed_along(value, axis, steps):
    count = lax.axis_size(axis)
    initial, last = (max(0, -steps), min(count, count - steps))
    return lax.ppermute(value, axis, [(source, source + steps) for source in range(initial, last)])


def slot_positions(route_block, n_experts, capacity):
    flat_ids = route_block.reshape(-1)
    onehot = (flat_ids[:, None] == jnp.arange(n_experts, dtype=jnp.int32)[None, :]).astype(
        jnp.int32
    )
    earlier = jnp.cumsum(onehot, axis=0) - onehot
    rank_in = jnp.sum(earlier * onehot, axis=1)
    return flat_ids * capacity + rank_in


def on_device(
    stream,
    pooled_in,
    pool_weight,
    pool_scale,
    out_weight,
    norm_gain,
    routes,
    route_weights,
    expert_gate,
    expert_up,
    expert_down,
    shared_gate,
    shared_up,
    shared_down,
):
    tok_dev, group_width = pooled_in.shape
    model_width = stream.shape[1]
    tp_size = lax.axis_size("tp")
    sp_size = lax.axis_size("sp")
    tp_index = lax.axis_index("tp")
    sp_index = lax.axis_index("sp")
    top_count = routes.shape[1]
    rows_dev = tok_dev // tp_size
    capacity = max(2, 2 * rows_dev * top_count // sp_size)
    window = lax.shift_left(jnp.int32(2), tp_index)
    rim_rows = passed_along(pooled_in[tok_dev - (REACH - 1) :], "sp", 1)
    padded = jnp.concatenate([rim_rows, pooled_in], 0).astype(jnp.float32)
    summed = jnp.zeros((tok_dev, group_width), jnp.float32)
    for lag_step in range(REACH):
        enabled = (lag_step < window).astype(jnp.float32)
        summed = summed + padded[REACH - 1 - lag_step : REACH - 1 - lag_step + tok_dev] * enabled
    position = sp_index * tok_dev + jnp.arange(tok_dev, dtype=jnp.int32)
    counted = jnp.minimum(position + 1, window).astype(jnp.float32)
    pooled = (summed / counted[:, None] - padded[REACH - 1 :]).astype(jnp.bfloat16)
    group_mix = (
        jnp.dot(pooled, pool_weight[0], preferred_element_type=jnp.float32) * pool_scale
    ).astype(jnp.bfloat16)
    mixed_all = jnp.dot(
        lax.all_gather(group_mix, "tp", axis=1, tiled=True),
        out_weight,
        preferred_element_type=jnp.float32,
    )
    residual = (stream.astype(jnp.float32) + mixed_all).astype(jnp.bfloat16)
    resid_wide = residual.astype(jnp.float32)
    normed = (
        resid_wide
        * lax.rsqrt(jnp.mean(resid_wide * resid_wide, axis=-1, keepdims=True) + EPSILON)
        * norm_gain
    ).astype(jnp.bfloat16)
    own_begin = tp_index * rows_dev
    own_routes = lax.dynamic_slice_in_dim(routes, own_begin, rows_dev, 0)
    own_pos = slot_positions(own_routes, sp_size, capacity)
    own_normed = lax.dynamic_slice_in_dim(normed, own_begin, rows_dev, 0)
    sending = jnp.zeros((sp_size * capacity, model_width), jnp.bfloat16)
    sending = sending.at[own_pos].set(jnp.repeat(own_normed, top_count, axis=0))
    landed = lax.all_to_all(
        sending.reshape(sp_size, capacity, model_width),
        "sp",
        split_axis=0,
        concat_axis=0,
        tiled=True,
    )
    arrived = lax.all_gather(landed[None], "tp", axis=0, tiled=True)
    arrived = arrived.reshape(-1, model_width)
    rows_in = arrived
    hidden = (
        jax.nn.silu(jnp.dot(rows_in, expert_gate[0], preferred_element_type=jnp.float32))
        * jnp.dot(rows_in, expert_up[0], preferred_element_type=jnp.float32)
    ).astype(jnp.bfloat16)
    expert_out = lax.psum_scatter(
        jnp.dot(hidden, expert_down[0], preferred_element_type=jnp.float32).astype(jnp.bfloat16),
        "tp",
        scatter_dimension=0,
        tiled=True,
    )
    returned = lax.all_to_all(
        expert_out.reshape(sp_size, capacity, model_width),
        "sp",
        split_axis=0,
        concat_axis=0,
        tiled=True,
    )
    picked = jnp.take(returned.reshape(-1, model_width), own_pos, axis=0)
    picked = picked.reshape(rows_dev, top_count, model_width)
    own_weights = lax.dynamic_slice_in_dim(route_weights, own_begin, rows_dev, 0)
    routed = jnp.sum(picked.astype(jnp.float32) * own_weights[:, :, None], axis=1)
    rows_in = normed
    hidden = (
        jax.nn.silu(jnp.dot(rows_in, shared_gate, preferred_element_type=jnp.float32))
        * jnp.dot(rows_in, shared_up, preferred_element_type=jnp.float32)
    ).astype(jnp.bfloat16)
    shared = lax.psum_scatter(
        jnp.dot(hidden, shared_down, preferred_element_type=jnp.float32).astype(jnp.bfloat16),
        "tp",
        scatter_dimension=0,
        tiled=True,
    ).astype(jnp.float32)
    own_resid = lax.dynamic_slice_in_dim(residual, own_begin, rows_dev, 0).astype(jnp.float32)
    return (own_resid + routed + shared).astype(jnp.bfloat16)


VMEM_ROOM = 40 * 2**20
LANES = 128


def exchange_kernel(
    nz,
    rows,
    width,
    pooled_ref,
    pmap_ref,
    pscale_ref,
    gain_ref,
    routes_ref,
    rweights_ref,
    stream_hbm,
    owt_hbm,
    gate_hbm,
    up_hbm,
    down_hbm,
    sgate_hbm,
    sup_hbm,
    sdown_hbm,
    out_ref,
    gbuf,
    acc,
    pbuf,
    rcbuf,
    sbuf_b,
    rbuf_b,
    sbuf_a,
    rbuf_a,
    sbuf_z,
    rbuf_z,
    hid,
    shid,
    wgate,
    wup,
    wdown,
    wsgate,
    wsup,
    wsdown,
    wout,
    resid,
    rim,
    gmix,
    mixbuf,
    wsem,
    rim_s,
    rim_r,
    mix_s,
    mix_r,
    zs,
    zr,
    a_s,
    a_r,
    bs,
    br,
    cs,
    cr,
    rcs,
    rcr,
    rbs,
    rbr,
    ras,
    rar,
    rzs,
    rzr,
):
    sp = lax.axis_index("sp")
    tp = lax.axis_index("tp")
    z, y = sp // 2, sp % 2
    x, c = tp // 2, tp % 2

    def dev(zz, yy, xx, cc):
        return (zz * 2 + yy, xx * 2 + cc)

    peer_a = dev(z, y + (1 - c) * (1 - 2 * y), x + c * (1 - 2 * x), c)
    peer_b = dev(z, y + c * (1 - 2 * y), x + (1 - c) * (1 - 2 * x), c)
    peer_c = dev(z, y, x, 1 - c)

    def peer_z(k):
        return dev((z + k) % nz, y, x, c)

    def rdma(src, dst, ssem, rsem, device):
        return pltpu.make_async_remote_copy(
            src_ref=src,
            dst_ref=dst,
            send_sem=ssem,
            recv_sem=rsem,
            device_id=device,
            device_id_type=pl.DeviceIdType.MESH,
        )

    def blk(cls, d, j):
        return gbuf.at[cls, d, pl.ds(j * rows, rows)]

    tok_dev = pooled_ref.shape[0]
    sp_size, tp_size = nz * 2, mixbuf.shape[0]
    own_rows = pl.ds(pl.multiple_of(tp * rows, rows), rows)
    weight_pairs = (
        (owt_hbm, wout),
        (stream_hbm.at[own_rows], resid),
        (gate_hbm.at[0], wgate),
        (up_hbm.at[0], wup),
        (down_hbm.at[0], wdown),
        (sgate_hbm, wsgate),
        (sup_hbm, wsup),
        (sdown_hbm, wsdown),
    )
    weight_copies = [
        pltpu.make_async_copy(s, t, wsem.at[i]) for i, (s, t) in enumerate(weight_pairs)
    ]
    for copy in weight_copies:
        copy.start()

    ahead = (sp + 1) % sp_size

    def rim_copy():
        last = pl.ds(tok_dev - REACH, REACH)
        return rdma(pooled_ref.at[last], rim, rim_s, rim_r, (ahead, tp))

    def mix_copy(k):
        there = (tp + k) % tp_size
        part = pl.ds(pl.multiple_of(there * rows, rows), rows)
        return rdma(gmix.at[part], mixbuf.at[tp], mix_s.at[k], mix_r.at[tp], (sp, there))

    def mix_recv(k):
        here = (tp + k) % tp_size
        return rdma(gmix.at[pl.ds(0, rows)], mixbuf.at[here], mix_s.at[k], mix_r.at[here], (sp, here))

    barrier = pltpu.get_barrier_semaphore()

    def greet(peer):
        pl.semaphore_signal(barrier, inc=1, device_id=peer, device_id_type=pl.DeviceIdType.MESH)

    peers = [peer_z(k) for k in range(1, nz)] + [dev(z, 1 - y, x, c)]
    peers = peers + [(sp, (tp + k) % tp_size) for k in range(1, tp_size)]
    slant = sp + 2 * y - 1
    slanted = (slant >= 0) & (slant < sp_size)
    for peer in peers:
        greet(peer)
    pl.when(slanted)(lambda: greet(((slant + sp_size) % sp_size, tp)))
    pl.semaphore_wait(barrier, len(peers) + jnp.where(slanted, 1, 0))

    near_first = [
        sorted(range(nz), key=lambda k: (abs(k - at), k if 2 * at < nz else -k))
        for at in range(nz)
    ]

    def source_at(at, slot):
        found = jnp.int32(0)
        for i in range(nz):
            for j in range(nz):
                found = jnp.where((at == i) & (slot == j), near_first[i][j], found)
        return found

    def slot_at(at, source):
        found = jnp.int32(0)
        for i in range(nz):
            for j in range(nz):
                found = jnp.where((at == i) & (source == j), near_first[i].index(j), found)
        return found

    def z_copy(slot, source, step):
        there = (z + step + nz) % nz
        landing = slot_at(there, source)
        index = 2 * slot + (1 if step > 0 else 0)
        return rdma(
            blk(0, slot, 0), blk(0, landing, 0), zs.at[index], zr.at[landing], dev(there, y, x, c)
        )

    def z_each(slot, act):
        source = z if isinstance(slot, int) and slot == 0 else source_at(z, slot)

        @pl.when((source <= z) & (z < nz - 1))
        def _():
            act(z_copy(slot, source, 1))

        @pl.when((source >= z) & (z > 0))
        def _():
            act(z_copy(slot, source, -1))

    def z_recv(d):
        return rdma(blk(0, 0, 0), blk(0, d, 0), zs.at[d], zr.at[d], peer_z(1))

    def a_copy(d):
        return rdma(blk(0, d, 0), blk(0, d, 1), a_s.at[d], a_r.at[d], peer_a)

    def b_copy(d, a):
        return rdma(blk(0, d, a), blk(0, d, 2 + a), bs.at[2 * d + a], br.at[2 * d + a], peer_b)

    def c_copy(d, j):
        return rdma(blk(0, d, j), blk(1, d, j), cs.at[4 * d + j], cr.at[4 * d + j], peer_c)

    def mixer():
        @pl.when(sp < sp_size - 1)
        def _():
            rim_copy().start()

        named = routes_ref[own_rows, :]
        given = rweights_ref[own_rows, :]
        lane = lax.broadcasted_iota(jnp.int32, (rows, LANES), 1)
        table = jnp.zeros((rows, LANES), jnp.float32)
        for k in range(named.shape[1]):
            hit = lane % (LANES // 2) == named[:, k : k + 1]
            table = table + jnp.where(hit, given[:, k : k + 1], 0.0)
        high = table.astype(jnp.bfloat16).astype(jnp.float32)
        tags = jnp.where(lane < LANES // 2, high, table - high).astype(jnp.bfloat16)
        gbuf[0, 0, 0:rows, width : width + LANES] = tags

        @pl.when(sp == 0)
        def _():
            rim[...] = jnp.zeros_like(rim)

        @pl.when(sp > 0)
        def _():
            rim_copy().wait_recv()

        own = pooled_ref[...].astype(jnp.float32)
        summed = jnp.concatenate([rim[...].astype(jnp.float32), own], 0)
        window = 2
        chosen = jnp.zeros_like(summed)
        for group in range(tp_size):
            summed = summed + pltpu.roll(summed, window // 2, 0)
            chosen = jnp.where(tp == group, summed, chosen)
            window = 2 * window
        mine = lax.shift_left(jnp.int32(2), tp)
        position = sp * tok_dev + lax.broadcasted_iota(jnp.int32, (tok_dev, 1), 0)
        counted = jnp.minimum(position + 1, mine).astype(jnp.float32)
        pooled = (chosen[REACH:] / counted - own).astype(jnp.bfloat16)
        mapped = jnp.dot(pooled, pmap_ref[0], preferred_element_type=jnp.float32)
        gmix[...] = (mapped * pscale_ref[...]).astype(jnp.bfloat16)
        for k in range(1, tp_size):
            mix_copy(k).start()
        mixbuf[tp] = gmix[own_rows, :]
        weight_copies[0].wait()
        weight_copies[1].wait()
        for k in range(1, tp_size):
            mix_recv(k).wait_recv()
        grouped = jnp.concatenate([mixbuf[k] for k in range(tp_size)], 1)
        squares = jnp.zeros((rows, 1), jnp.float32)
        step = min(512, width)
        for i in range(width // step):
            cols = slice(i * step, (i + 1) * step)
            mixed = jnp.dot(grouped, wout[:, cols], preferred_element_type=jnp.float32)
            after = (resid[:, cols].astype(jnp.float32) + mixed).astype(jnp.bfloat16)
            resid[:, cols] = after
            after = after.astype(jnp.float32)
            squares = squares + jnp.sum(after * after, axis=1, keepdims=True)
        factor = lax.rsqrt(squares / width + EPSILON)
        for i in range(width // step):
            cols = slice(i * step, (i + 1) * step)
            normed = resid[:, cols].astype(jnp.float32) * factor * gain_ref[:, cols]
            gbuf[0, 0, 0:rows, cols] = normed.astype(jnp.bfloat16)

    def first_pass(d):
        a_copy(d).start()
        b_copy(d, 0).start()
        c_copy(d, 0).start()

    def second_pass(d):
        a_copy(d).wait_recv()
        b_copy(d, 1).start()
        c_copy(d, 1).start()

    def rc_copy(d):
        return rdma(pbuf.at[d], rcbuf.at[d], rcs.at[d], rcr.at[d], peer_c)

    def rb_copy(d, a):
        part = pl.ds(a * rows, rows)
        sems = rbs.at[2 * d + a], rbr.at[2 * d + a]
        return rdma(sbuf_b.at[d, part], rbuf_b.at[d, part], *sems, peer_b)

    def ra_copy(d):
        return rdma(sbuf_a.at[d], rbuf_a.at[d], ras.at[d], rar.at[d], peer_a)

    def rz_copy(d):
        there = source_at(z, d)
        landing = slot_at(there, z)
        return rdma(
            sbuf_z.at[d], rbuf_z.at[landing], rzs.at[d], rzr.at[landing], dev(there, y, x, c)
        )

    def rz_recv(d):
        return rdma(sbuf_z.at[d], rbuf_z.at[d], rzs.at[d], rzr.at[d], peer_z(1))

    dot = functools.partial(jnp.dot, preferred_element_type=jnp.float32)
    step_in = min(256, wgate.shape[1])
    step_out = min(512, width)

    def hidden_of(cls, d, gate, up, result, step):
        @pl.loop(0, gate.shape[1] // step)
        def _(i):
            cols = pl.ds(pl.multiple_of(i * step, step), step)
            block = gbuf[cls, d, :, 0:width]
            g = dot(block, gate[:, cols])
            u = dot(block, up[:, cols])
            result[:, cols] = (g / (1.0 + jnp.exp(-g)) * u).astype(jnp.bfloat16)

    def expert(cls, d, store):
        hidden_of(cls, d, wgate, wup, hid, step_in)
        tags = gbuf[cls, d, :, width : width + LANES].astype(jnp.float32)
        lane = lax.broadcasted_iota(jnp.int32, tags.shape, 1)
        mine = (lane == sp) | (lane == sp + LANES // 2)
        weight = jnp.sum(jnp.where(mine, tags, 0.0), axis=1, keepdims=True)

        @pl.when(d > 0)
        def _():
            @pl.loop(0, width // step_out)
            def _(i):
                cols = pl.ds(pl.multiple_of(i * step_out, step_out), step_out)
                store(cols, dot(hid[...], wdown[:, cols]) * weight)

        @pl.when(d == 0)
        def _():
            hidden_of(cls, d, wsgate, wsup, shid, wsgate.shape[1])
            group = lax.broadcasted_iota(jnp.int32, weight.shape, 0) // rows
            flag = jnp.where((c + cls) % 2 == 0, group % 2, group // 2)
            near = jnp.where(flag == 0, 1.0, 0.0)

            @pl.loop(0, width // step_out)
            def _(i):
                cols = pl.ds(pl.multiple_of(i * step_out, step_out), step_out)
                store(
                    cols,
                    dot(hid[...], wdown[:, cols]) * weight
                    + dot(shid[...], wsdown[:, cols]) * near,
                )

    def wide(value):
        return value.astype(jnp.float32)

    def reduce_b(d):
        rc_copy(d).wait_recv()
        for a in (1, 0):
            here = pl.ds(a * rows, rows)
            part = pl.ds((2 + a) * rows, rows)
            total = acc[d, part, :] + wide(rcbuf[d, part, :])
            sbuf_b[d, here, :] = total.astype(jnp.bfloat16)
            rb_copy(d, a).start()

    def reduce_a(d):
        rb_copy(d, 1).wait_recv()
        part = pl.ds(rows, rows)
        total = acc[d, part, :] + wide(rcbuf[d, part, :]) + wide(rbuf_b[d, part, :])
        sbuf_a[d] = total.astype(jnp.bfloat16)
        ra_copy(d).start()

    def base_total(d):
        part = pl.ds(0, rows)
        return (
            acc[d, part, :]
            + wide(rcbuf[d, part, :])
            + wide(rbuf_b[d, part, :])
            + wide(rbuf_a[d])
        )

    def reduce_z(d):
        rb_copy(d, 0).wait_recv()
        ra_copy(d).wait_recv()

        @pl.when(d > 0)
        def _():
            send_z(d)

    def send_z(d):
        sbuf_z[d] = base_total(d).astype(jnp.bfloat16)
        rz_copy(d).start()

    def z_arrival(d):
        z_recv(d).wait_recv()
        z_each(d, lambda copy: copy.start())
        first_pass(d)

    def b_arrival(d):
        for a in range(2):
            b_copy(d, a).wait_recv()
            c_copy(d, 2 + a).start()

    mixer()
    z_each(0, lambda copy: copy.start())
    first_pass(0)
    z_arrival(1)
    second_pass(0)
    b_arrival(0)
    for copy in weight_copies[2:]:
        copy.wait()

    @pl.loop(0, nz)
    def _(d):
        @pl.when(d + 2 < nz)
        def _():
            z_arrival(d + 2)

        @pl.when(d + 1 < nz)
        def _():
            second_pass(d + 1)

        for j in range(4):
            c_copy(d, j).wait_recv()

        def store_part(cols, value):
            pbuf[d, :, cols] = value.astype(jnp.bfloat16)

        expert(1, d, store_part)
        rc_copy(d).start()

        def store_acc(cols, value):
            acc[d, :, cols] = value

        expert(0, d, store_acc)
        reduce_b(d)

        @pl.when(d + 1 < nz)
        def _():
            b_arrival(d + 1)

        @pl.when(d >= 1)
        def _():
            reduce_a(d - 1)

        @pl.when(d >= 2)
        def _():
            reduce_z(d - 2)

    reduce_a(nz - 1)
    reduce_z(nz - 2)
    reduce_z(nz - 1)
    total = base_total(0) + wide(resid[...])
    for d in range(1, nz):
        rz_recv(d).wait_recv()
        total = total + wide(rbuf_z[d])
    out_ref[...] = total.astype(jnp.bfloat16)

    pl.when(sp < sp_size - 1)(lambda: rim_copy().wait_send())
    for k in range(1, tp_size):
        mix_copy(k).wait_send()
    for k in range(1, nz):
        rz_copy(k).wait_send()

    z_each(0, lambda copy: copy.wait_send())
    for k in range(1, nz):
        z_each(k, lambda copy: copy.wait_send())

    @pl.loop(0, nz)
    def _(d):
        a_copy(d).wait_send()
        for a in range(2):
            b_copy(d, a).wait_send()
            rb_copy(d, a).wait_send()
        for j in range(4):
            c_copy(d, j).wait_send()
        rc_copy(d).wait_send()
        ra_copy(d).wait_send()


def exchanged(small, large, rows, nz):
    pooled_in = small[0]
    stream, out_weight, gate, up, down, sgate, sup, sdown = large
    width = stream.shape[1]
    tok_dev, group_width = pooled_in.shape
    bf16, f32 = jnp.bfloat16, jnp.float32
    four, two = 4 * rows, 2 * rows
    vm = pltpu.VMEM
    dma = pltpu.SemaphoreType.DMA
    any_spec = pl.BlockSpec(memory_space=pl.ANY)
    vmem_spec = pl.BlockSpec(memory_space=pltpu.VMEM)
    return pl.pallas_call(
        functools.partial(exchange_kernel, nz, rows, width),
        out_shape=jax.ShapeDtypeStruct((rows, width), bf16),
        in_specs=[vmem_spec] * len(small) + [any_spec] * len(large),
        out_specs=vmem_spec,
        scratch_shapes=[
            vm((2, nz, four, width + LANES), bf16),
            vm((nz, four, width), f32),
            vm((nz, four, width), bf16),
            vm((nz, four, width), bf16),
            vm((nz, two, width), bf16),
            vm((nz, two, width), bf16),
            vm((nz, rows, width), bf16),
            vm((nz, rows, width), bf16),
            vm((nz, rows, width), bf16),
            vm((nz, rows, width), bf16),
            vm((four, gate.shape[2]), bf16),
            vm((four, sgate.shape[1]), bf16),
            vm(gate.shape[1:], bf16),
            vm(up.shape[1:], bf16),
            vm(down.shape[1:], bf16),
            vm(sgate.shape, bf16),
            vm(sup.shape, bf16),
            vm(sdown.shape, bf16),
            vm(out_weight.shape, bf16),
            vm((rows, width), bf16),
            vm((REACH, group_width), bf16),
            vm((tok_dev, group_width), bf16),
            vm((tok_dev // rows, rows, group_width), bf16),
            dma((len(large),)),
            dma,
            dma,
            dma((tok_dev // rows,)),
            dma((tok_dev // rows,)),
        ]
        + [dma((n,)) for n in (2 * nz, nz, nz, nz, 2 * nz, 2 * nz, 4 * nz, 4 * nz)]
        + [dma((n,)) for n in (nz, nz, 2 * nz, 2 * nz, nz, nz, nz, nz)],
        compiler_params=pltpu.CompilerParams(
            collective_id=0, has_side_effects=True, vmem_limit_bytes=60 * 2**20
        ),
        name="exchange_experts",
    )(*small, *large)


def on_device_dense(
    stream,
    pooled_in,
    pool_weight,
    pool_scale,
    out_weight,
    norm_gain,
    routes,
    route_weights,
    expert_gate,
    expert_up,
    expert_down,
    shared_gate,
    shared_up,
    shared_down,
):
    nz = lax.axis_size("sp") // 2
    rows_dev = pooled_in.shape[0] // lax.axis_size("tp")
    small = (pooled_in, pool_weight, pool_scale[None], norm_gain[None], routes, route_weights)
    large = (stream, out_weight, expert_gate, expert_up, expert_down)
    return exchanged(small, large + (shared_gate, shared_up, shared_down), rows_dev, nz)


def held_whole(mesh, *args):
    stream, expert_gate = args[0], args[8]
    sp_size, tp_size = mesh.shape["sp"], mesh.shape["tp"]
    return (
        3 * stream.size * stream.dtype.itemsize <= VMEM_ROOM
        and sp_size % 2 == 0
        and sp_size <= LANES // 2
        and tp_size == WINDOW_GROUPS
        and expert_gate.shape[0] == sp_size
    )


def solution(mesh):
    placed = (
        P("sp", None),
        P("sp", "tp"),
        P("tp", None, None),
        P("tp"),
        P(),
        P(),
        P("sp", None),
        P("sp", None),
        P("sp", None, "tp"),
        P("sp", None, "tp"),
        P("sp", "tp", None),
        P(None, "tp"),
        P(None, "tp"),
        P("tp", None),
    )

    def layer(*args):
        body = on_device_dense if held_whole(mesh, *args) else on_device
        return jax.shard_map(
            body, mesh=mesh, in_specs=placed, out_specs=P(("sp", "tp"), None), check_vma=False
        )(*args)

    return layer
```

```python
import functools
import jax
import jax.numpy as jnp
from jax import lax
from jax.experimental import pallas as pl
from jax.experimental.pallas import tpu as pltpu
from jax.sharding import PartitionSpec as P

REACH = 16


EPSILON = 1e-06
WINDOW_GROUPS = 4


def passed_along(value, axis, steps):
    count = lax.axis_size(axis)
    initial, last = (max(0, -steps), min(count, count - steps))
    return lax.ppermute(value, axis, [(source, source + steps) for source in range(initial, last)])


def slot_positions(route_block, n_experts, capacity):
    flat_ids = route_block.reshape(-1)
    onehot = (flat_ids[:, None] == jnp.arange(n_experts, dtype=jnp.int32)[None, :]).astype(
        jnp.int32
    )
    earlier = jnp.cumsum(onehot, axis=0) - onehot
    rank_in = jnp.sum(earlier * onehot, axis=1)
    return flat_ids * capacity + rank_in


def on_device(
    stream,
    pooled_in,
    pool_weight,
    pool_scale,
    out_weight,
    norm_gain,
    routes,
    route_weights,
    expert_gate,
    expert_up,
    expert_down,
    shared_gate,
    shared_up,
    shared_down,
):
    tok_dev, group_width = pooled_in.shape
    model_width = stream.shape[1]
    tp_size = lax.axis_size("tp")
    sp_size = lax.axis_size("sp")
    tp_index = lax.axis_index("tp")
    sp_index = lax.axis_index("sp")
    top_count = routes.shape[1]
    rows_dev = tok_dev // tp_size
    capacity = max(2, 2 * rows_dev * top_count // sp_size)
    window = lax.shift_left(jnp.int32(2), tp_index)
    rim_rows = passed_along(pooled_in[tok_dev - (REACH - 1) :], "sp", 1)
    padded = jnp.concatenate([rim_rows, pooled_in], 0).astype(jnp.float32)
    summed = jnp.zeros((tok_dev, group_width), jnp.float32)
    for lag_step in range(REACH):
        enabled = (lag_step < window).astype(jnp.float32)
        summed = summed + padded[REACH - 1 - lag_step : REACH - 1 - lag_step + tok_dev] * enabled
    position = sp_index * tok_dev + jnp.arange(tok_dev, dtype=jnp.int32)
    counted = jnp.minimum(position + 1, window).astype(jnp.float32)
    pooled = (summed / counted[:, None] - padded[REACH - 1 :]).astype(jnp.bfloat16)
    group_mix = (
        jnp.dot(pooled, pool_weight[0], preferred_element_type=jnp.float32) * pool_scale
    ).astype(jnp.bfloat16)
    mixed_all = jnp.dot(
        lax.all_gather(group_mix, "tp", axis=1, tiled=True),
        out_weight,
        preferred_element_type=jnp.float32,
    )
    residual = (stream.astype(jnp.float32) + mixed_all).astype(jnp.bfloat16)
    resid_wide = residual.astype(jnp.float32)
    normed = (
        resid_wide
        * lax.rsqrt(jnp.mean(resid_wide * resid_wide, axis=-1, keepdims=True) + EPSILON)
        * norm_gain
    ).astype(jnp.bfloat16)
    own_begin = tp_index * rows_dev
    own_routes = lax.dynamic_slice_in_dim(routes, own_begin, rows_dev, 0)
    own_pos = slot_positions(own_routes, sp_size, capacity)
    own_normed = lax.dynamic_slice_in_dim(normed, own_begin, rows_dev, 0)
    sending = jnp.zeros((sp_size * capacity, model_width), jnp.bfloat16)
    sending = sending.at[own_pos].set(jnp.repeat(own_normed, top_count, axis=0))
    landed = lax.all_to_all(
        sending.reshape(sp_size, capacity, model_width),
        "sp",
        split_axis=0,
        concat_axis=0,
        tiled=True,
    )
    arrived = lax.all_gather(landed[None], "tp", axis=0, tiled=True)
    arrived = arrived.reshape(-1, model_width)
    rows_in = arrived
    hidden = (
        jax.nn.silu(jnp.dot(rows_in, expert_gate[0], preferred_element_type=jnp.float32))
        * jnp.dot(rows_in, expert_up[0], preferred_element_type=jnp.float32)
    ).astype(jnp.bfloat16)
    expert_out = lax.psum_scatter(
        jnp.dot(hidden, expert_down[0], preferred_element_type=jnp.float32).astype(jnp.bfloat16),
        "tp",
        scatter_dimension=0,
        tiled=True,
    )
    returned = lax.all_to_all(
        expert_out.reshape(sp_size, capacity, model_width),
        "sp",
        split_axis=0,
        concat_axis=0,
        tiled=True,
    )
    picked = jnp.take(returned.reshape(-1, model_width), own_pos, axis=0)
    picked = picked.reshape(rows_dev, top_count, model_width)
    own_weights = lax.dynamic_slice_in_dim(route_weights, own_begin, rows_dev, 0)
    routed = jnp.sum(picked.astype(jnp.float32) * own_weights[:, :, None], axis=1)
    rows_in = normed
    hidden = (
        jax.nn.silu(jnp.dot(rows_in, shared_gate, preferred_element_type=jnp.float32))
        * jnp.dot(rows_in, shared_up, preferred_element_type=jnp.float32)
    ).astype(jnp.bfloat16)
    shared = lax.psum_scatter(
        jnp.dot(hidden, shared_down, preferred_element_type=jnp.float32).astype(jnp.bfloat16),
        "tp",
        scatter_dimension=0,
        tiled=True,
    ).astype(jnp.float32)
    own_resid = lax.dynamic_slice_in_dim(residual, own_begin, rows_dev, 0).astype(jnp.float32)
    return (own_resid + routed + shared).astype(jnp.bfloat16)


VMEM_ROOM = 40 * 2**20
LANES = 128


def exchange_kernel(
    nz,
    rows,
    width,
    pooled_ref,
    pmap_ref,
    pscale_ref,
    gain_ref,
    routes_ref,
    rweights_ref,
    stream_hbm,
    owt_hbm,
    gate_hbm,
    up_hbm,
    down_hbm,
    sgate_hbm,
    sup_hbm,
    sdown_hbm,
    out_ref,
    gbuf,
    acc,
    pbuf,
    rcbuf,
    sbuf_b,
    rbuf_b,
    sbuf_a,
    rbuf_a,
    sbuf_z,
    rbuf_z,
    hid,
    shid,
    wgate,
    wup,
    wdown,
    wsgate,
    wsup,
    wsdown,
    wout,
    resid,
    rim,
    gmix,
    mixbuf,
    wsem,
    rim_s,
    rim_r,
    mix_s,
    mix_r,
    zs,
    zr,
    a_s,
    a_r,
    bs,
    br,
    cs,
    cr,
    rcs,
    rcr,
    rbs,
    rbr,
    ras,
    rar,
    rzs,
    rzr,
):
    sp = lax.axis_index("sp")
    tp = lax.axis_index("tp")
    z, y = sp // 2, sp % 2
    x, c = tp // 2, tp % 2

    def dev(zz, yy, xx, cc):
        return (zz * 2 + yy, xx * 2 + cc)

    peer_a = dev(z, y + (1 - c) * (1 - 2 * y), x + c * (1 - 2 * x), c)
    peer_b = dev(z, y + c * (1 - 2 * y), x + (1 - c) * (1 - 2 * x), c)
    peer_c = dev(z, y, x, 1 - c)

    def peer_z(k):
        return dev((z + k) % nz, y, x, c)

    def rdma(src, dst, ssem, rsem, device):
        return pltpu.make_async_remote_copy(
            src_ref=src,
            dst_ref=dst,
            send_sem=ssem,
            recv_sem=rsem,
            device_id=device,
            device_id_type=pl.DeviceIdType.MESH,
        )

    def blk(cls, d, j):
        return gbuf.at[cls, d, pl.ds(j * rows, rows)]

    tok_dev = pooled_ref.shape[0]
    sp_size, tp_size = nz * 2, mixbuf.shape[0]
    own_rows = pl.ds(pl.multiple_of(tp * rows, rows), rows)
    weight_pairs = (
        (owt_hbm, wout),
        (stream_hbm.at[own_rows], resid),
        (gate_hbm.at[0], wgate),
        (up_hbm.at[0], wup),
        (down_hbm.at[0], wdown),
        (sgate_hbm, wsgate),
        (sup_hbm, wsup),
        (sdown_hbm, wsdown),
    )
    weight_copies = [
        pltpu.make_async_copy(s, t, wsem.at[i]) for i, (s, t) in enumerate(weight_pairs)
    ]
    for copy in weight_copies:
        copy.start()

    ahead = (sp + 1) % sp_size

    def rim_copy():
        last = pl.ds(tok_dev - REACH, REACH)
        return rdma(pooled_ref.at[last], rim, rim_s, rim_r, (ahead, tp))

    def mix_copy(k):
        there = (tp + k) % tp_size
        part = pl.ds(pl.multiple_of(there * rows, rows), rows)
        return rdma(gmix.at[part], mixbuf.at[tp], mix_s.at[k], mix_r.at[tp], (sp, there))

    def mix_recv(k):
        here = (tp + k) % tp_size
        return rdma(gmix.at[pl.ds(0, rows)], mixbuf.at[here], mix_s.at[k], mix_r.at[here], (sp, here))

    barrier = pltpu.get_barrier_semaphore()

    def greet(peer):
        pl.semaphore_signal(barrier, inc=1, device_id=peer, device_id_type=pl.DeviceIdType.MESH)

    peers = [peer_z(k) for k in range(1, nz)] + [dev(z, 1 - y, x, c)]
    peers = peers + [(sp, (tp + k) % tp_size) for k in range(1, tp_size)]
    slant = sp + 2 * y - 1
    slanted = (slant >= 0) & (slant < sp_size)
    for peer in peers:
        greet(peer)
    pl.when(slanted)(lambda: greet(((slant + sp_size) % sp_size, tp)))
    pl.semaphore_wait(barrier, len(peers) + jnp.where(slanted, 1, 0))

    far_first = [
        sorted(range(nz), key=lambda k: (k != at, -abs(k - at), k))
        for at in range(nz)
    ]

    def source_at(at, slot):
        found = jnp.int32(0)
        for i in range(nz):
            for j in range(nz):
                found = jnp.where((at == i) & (slot == j), far_first[i][j], found)
        return found

    def slot_at(at, source):
        found = jnp.int32(0)
        for i in range(nz):
            for j in range(nz):
                found = jnp.where((at == i) & (source == j), far_first[i].index(j), found)
        return found

    def z_copy(d):
        there = source_at(z, d)
        landing = slot_at(there, z)
        return rdma(
            blk(0, 0, 0), blk(0, landing, 0), zs.at[d], zr.at[landing], dev(there, y, x, c)
        )

    def z_recv(d):
        return rdma(blk(0, 0, 0), blk(0, d, 0), zs.at[d], zr.at[d], peer_z(1))

    def a_copy(d):
        return rdma(blk(0, d, 0), blk(0, d, 1), a_s.at[d], a_r.at[d], peer_a)

    def b_copy(d, a):
        return rdma(blk(0, d, a), blk(0, d, 2 + a), bs.at[2 * d + a], br.at[2 * d + a], peer_b)

    def c_copy(d, j):
        return rdma(blk(0, d, j), blk(1, d, j), cs.at[4 * d + j], cr.at[4 * d + j], peer_c)

    def mixer():
        @pl.when(sp < sp_size - 1)
        def _():
            rim_copy().start()

        named = routes_ref[own_rows, :]
        given = rweights_ref[own_rows, :]
        lane = lax.broadcasted_iota(jnp.int32, (rows, LANES), 1)
        table = jnp.zeros((rows, LANES), jnp.float32)
        for k in range(named.shape[1]):
            hit = lane % (LANES // 2) == named[:, k : k + 1]
            table = table + jnp.where(hit, given[:, k : k + 1], 0.0)
        high = table.astype(jnp.bfloat16).astype(jnp.float32)
        tags = jnp.where(lane < LANES // 2, high, table - high).astype(jnp.bfloat16)
        gbuf[0, 0, 0:rows, width : width + LANES] = tags

        @pl.when(sp == 0)
        def _():
            rim[...] = jnp.zeros_like(rim)

        @pl.when(sp > 0)
        def _():
            rim_copy().wait_recv()

        own = pooled_ref[...].astype(jnp.float32)
        summed = jnp.concatenate([rim[...].astype(jnp.float32), own], 0)
        window = 2
        chosen = jnp.zeros_like(summed)
        for group in range(tp_size):
            summed = summed + pltpu.roll(summed, window // 2, 0)
            chosen = jnp.where(tp == group, summed, chosen)
            window = 2 * window
        mine = lax.shift_left(jnp.int32(2), tp)
        position = sp * tok_dev + lax.broadcasted_iota(jnp.int32, (tok_dev, 1), 0)
        counted = jnp.minimum(position + 1, mine).astype(jnp.float32)
        pooled = (chosen[REACH:] / counted - own).astype(jnp.bfloat16)
        mapped = jnp.dot(pooled, pmap_ref[0], preferred_element_type=jnp.float32)
        gmix[...] = (mapped * pscale_ref[...]).astype(jnp.bfloat16)
        for k in range(1, tp_size):
            mix_copy(k).start()
        mixbuf[tp] = gmix[own_rows, :]
        weight_copies[0].wait()
        weight_copies[1].wait()
        for k in range(1, tp_size):
            mix_recv(k).wait_recv()
        grouped = jnp.concatenate([mixbuf[k] for k in range(tp_size)], 1)
        squares = jnp.zeros((rows, 1), jnp.float32)
        step = min(512, width)
        for i in range(width // step):
            cols = slice(i * step, (i + 1) * step)
            mixed = jnp.dot(grouped, wout[:, cols], preferred_element_type=jnp.float32)
            after = (resid[:, cols].astype(jnp.float32) + mixed).astype(jnp.bfloat16)
            resid[:, cols] = after
            after = after.astype(jnp.float32)
            squares = squares + jnp.sum(after * after, axis=1, keepdims=True)
        factor = lax.rsqrt(squares / width + EPSILON)
        for i in range(width // step):
            cols = slice(i * step, (i + 1) * step)
            normed = resid[:, cols].astype(jnp.float32) * factor * gain_ref[:, cols]
            gbuf[0, 0, 0:rows, cols] = normed.astype(jnp.bfloat16)

    def first_pass(d):
        a_copy(d).start()
        b_copy(d, 0).start()
        c_copy(d, 0).start()

    def second_pass(d):
        a_copy(d).wait_recv()
        b_copy(d, 1).start()
        c_copy(d, 1).start()

    def rc_copy(d):
        return rdma(pbuf.at[d], rcbuf.at[d], rcs.at[d], rcr.at[d], peer_c)

    def rb_copy(d, a):
        part = pl.ds(a * rows, rows)
        sems = rbs.at[2 * d + a], rbr.at[2 * d + a]
        return rdma(sbuf_b.at[d, part], rbuf_b.at[d, part], *sems, peer_b)

    def ra_copy(d):
        return rdma(sbuf_a.at[d], rbuf_a.at[d], ras.at[d], rar.at[d], peer_a)

    def rz_copy(d):
        there = source_at(z, d)
        landing = slot_at(there, z)
        return rdma(
            sbuf_z.at[d], rbuf_z.at[landing], rzs.at[d], rzr.at[landing], dev(there, y, x, c)
        )

    def rz_recv(d):
        return rdma(sbuf_z.at[d], rbuf_z.at[d], rzs.at[d], rzr.at[d], peer_z(1))

    dot = functools.partial(jnp.dot, preferred_element_type=jnp.float32)
    step_in = min(256, wgate.shape[1])
    step_out = min(512, width)

    def hidden_of(cls, d, gate, up, result, step):
        @pl.loop(0, gate.shape[1] // step)
        def _(i):
            cols = pl.ds(pl.multiple_of(i * step, step), step)
            block = gbuf[cls, d, :, 0:width]
            g = dot(block, gate[:, cols])
            u = dot(block, up[:, cols])
            result[:, cols] = (g / (1.0 + jnp.exp(-g)) * u).astype(jnp.bfloat16)

    def expert(cls, d, store):
        hidden_of(cls, d, wgate, wup, hid, step_in)
        tags = gbuf[cls, d, :, width : width + LANES].astype(jnp.float32)
        lane = lax.broadcasted_iota(jnp.int32, tags.shape, 1)
        mine = (lane == sp) | (lane == sp + LANES // 2)
        weight = jnp.sum(jnp.where(mine, tags, 0.0), axis=1, keepdims=True)

        @pl.when(d > 0)
        def _():
            @pl.loop(0, width // step_out)
            def _(i):
                cols = pl.ds(pl.multiple_of(i * step_out, step_out), step_out)
                store(cols, dot(hid[...], wdown[:, cols]) * weight)

        @pl.when(d == 0)
        def _():
            hidden_of(cls, d, wsgate, wsup, shid, wsgate.shape[1])
            group = lax.broadcasted_iota(jnp.int32, weight.shape, 0) // rows
            flag = jnp.where((c + cls) % 2 == 0, group % 2, group // 2)
            near = jnp.where(flag == 0, 1.0, 0.0)

            @pl.loop(0, width // step_out)
            def _(i):
                cols = pl.ds(pl.multiple_of(i * step_out, step_out), step_out)
                store(
                    cols,
                    dot(hid[...], wdown[:, cols]) * weight
                    + dot(shid[...], wsdown[:, cols]) * near,
                )

    def wide(value):
        return value.astype(jnp.float32)

    def reduce_b(d):
        rc_copy(d).wait_recv()
        for a in (1, 0):
            here = pl.ds(a * rows, rows)
            part = pl.ds((2 + a) * rows, rows)
            total = acc[d, part, :] + wide(rcbuf[d, part, :])
            sbuf_b[d, here, :] = total.astype(jnp.bfloat16)
            rb_copy(d, a).start()

    def reduce_a(d):
        rb_copy(d, 1).wait_recv()
        part = pl.ds(rows, rows)
        total = acc[d, part, :] + wide(rcbuf[d, part, :]) + wide(rbuf_b[d, part, :])
        sbuf_a[d] = total.astype(jnp.bfloat16)
        ra_copy(d).start()

    def base_total(d):
        part = pl.ds(0, rows)
        return (
            acc[d, part, :]
            + wide(rcbuf[d, part, :])
            + wide(rbuf_b[d, part, :])
            + wide(rbuf_a[d])
        )

    def reduce_z(d):
        rb_copy(d, 0).wait_recv()
        ra_copy(d).wait_recv()

        @pl.when(d > 0)
        def _():
            send_z(d)

    def send_z(d):
        sbuf_z[d] = base_total(d).astype(jnp.bfloat16)
        rz_copy(d).start()

    def z_arrival(d):
        z_recv(d).wait_recv()
        first_pass(d)

    def b_arrival(d):
        for a in range(2):
            b_copy(d, a).wait_recv()
            c_copy(d, 2 + a).start()

    mixer()
    for k in range(1, nz):
        z_copy(k).start()
    first_pass(0)
    z_arrival(1)
    second_pass(0)
    b_arrival(0)
    for copy in weight_copies[2:]:
        copy.wait()

    @pl.loop(0, nz)
    def _(d):
        @pl.when(d + 2 < nz)
        def _():
            z_arrival(d + 2)

        @pl.when(d + 1 < nz)
        def _():
            second_pass(d + 1)

        for j in range(4):
            c_copy(d, j).wait_recv()

        def store_part(cols, value):
            pbuf[d, :, cols] = value.astype(jnp.bfloat16)

        expert(1, d, store_part)
        rc_copy(d).start()

        def store_acc(cols, value):
            acc[d, :, cols] = value

        expert(0, d, store_acc)
        reduce_b(d)

        @pl.when(d + 1 < nz)
        def _():
            b_arrival(d + 1)

        @pl.when(d >= 1)
        def _():
            reduce_a(d - 1)

        @pl.when(d >= 2)
        def _():
            reduce_z(d - 2)

    reduce_a(nz - 1)
    reduce_z(nz - 2)
    reduce_z(nz - 1)
    total = base_total(0) + wide(resid[...])
    for d in range(1, nz):
        rz_recv(d).wait_recv()
        total = total + wide(rbuf_z[d])
    out_ref[...] = total.astype(jnp.bfloat16)

    pl.when(sp < sp_size - 1)(lambda: rim_copy().wait_send())
    for k in range(1, tp_size):
        mix_copy(k).wait_send()
    for k in range(1, nz):
        rz_copy(k).wait_send()

    for k in range(1, nz):
        z_copy(k).wait_send()

    @pl.loop(0, nz)
    def _(d):
        a_copy(d).wait_send()
        for a in range(2):
            b_copy(d, a).wait_send()
            rb_copy(d, a).wait_send()
        for j in range(4):
            c_copy(d, j).wait_send()
        rc_copy(d).wait_send()
        ra_copy(d).wait_send()


def exchanged(small, large, rows, nz):
    pooled_in = small[0]
    stream, out_weight, gate, up, down, sgate, sup, sdown = large
    width = stream.shape[1]
    tok_dev, group_width = pooled_in.shape
    bf16, f32 = jnp.bfloat16, jnp.float32
    four, two = 4 * rows, 2 * rows
    vm = pltpu.VMEM
    dma = pltpu.SemaphoreType.DMA
    any_spec = pl.BlockSpec(memory_space=pl.ANY)
    vmem_spec = pl.BlockSpec(memory_space=pltpu.VMEM)
    return pl.pallas_call(
        functools.partial(exchange_kernel, nz, rows, width),
        out_shape=jax.ShapeDtypeStruct((rows, width), bf16),
        in_specs=[vmem_spec] * len(small) + [any_spec] * len(large),
        out_specs=vmem_spec,
        scratch_shapes=[
            vm((2, nz, four, width + LANES), bf16),
            vm((nz, four, width), f32),
            vm((nz, four, width), bf16),
            vm((nz, four, width), bf16),
            vm((nz, two, width), bf16),
            vm((nz, two, width), bf16),
            vm((nz, rows, width), bf16),
            vm((nz, rows, width), bf16),
            vm((nz, rows, width), bf16),
            vm((nz, rows, width), bf16),
            vm((four, gate.shape[2]), bf16),
            vm((four, sgate.shape[1]), bf16),
            vm(gate.shape[1:], bf16),
            vm(up.shape[1:], bf16),
            vm(down.shape[1:], bf16),
            vm(sgate.shape, bf16),
            vm(sup.shape, bf16),
            vm(sdown.shape, bf16),
            vm(out_weight.shape, bf16),
            vm((rows, width), bf16),
            vm((REACH, group_width), bf16),
            vm((tok_dev, group_width), bf16),
            vm((tok_dev // rows, rows, group_width), bf16),
            dma((len(large),)),
            dma,
            dma,
            dma((tok_dev // rows,)),
            dma((tok_dev // rows,)),
        ]
        + [dma((n,)) for n in (nz, nz, nz, nz, 2 * nz, 2 * nz, 4 * nz, 4 * nz)]
        + [dma((n,)) for n in (nz, nz, 2 * nz, 2 * nz, nz, nz, nz, nz)],
        compiler_params=pltpu.CompilerParams(
            collective_id=0, has_side_effects=True, vmem_limit_bytes=60 * 2**20
        ),
        name="exchange_experts",
    )(*small, *large)


def on_device_dense(
    stream,
    pooled_in,
    pool_weight,
    pool_scale,
    out_weight,
    norm_gain,
    routes,
    route_weights,
    expert_gate,
    expert_up,
    expert_down,
    shared_gate,
    shared_up,
    shared_down,
):
    nz = lax.axis_size("sp") // 2
    rows_dev = pooled_in.shape[0] // lax.axis_size("tp")
    small = (pooled_in, pool_weight, pool_scale[None], norm_gain[None], routes, route_weights)
    large = (stream, out_weight, expert_gate, expert_up, expert_down)
    return exchanged(small, large + (shared_gate, shared_up, shared_down), rows_dev, nz)


def held_whole(mesh, *args):
    stream, expert_gate = args[0], args[8]
    sp_size, tp_size = mesh.shape["sp"], mesh.shape["tp"]
    return (
        3 * stream.size * stream.dtype.itemsize <= VMEM_ROOM
        and sp_size % 2 == 0
        and sp_size <= LANES // 2
        and tp_size == WINDOW_GROUPS
        and expert_gate.shape[0] == sp_size
    )


def solution(mesh):
    placed = (
        P("sp", None),
        P("sp", "tp"),
        P("tp", None, None),
        P("tp"),
        P(),
        P(),
        P("sp", None),
        P("sp", None),
        P("sp", None, "tp"),
        P("sp", None, "tp"),
        P("sp", "tp", None),
        P(None, "tp"),
        P(None, "tp"),
        P("tp", None),
    )

    def layer(*args):
        body = on_device_dense if held_whole(mesh, *args) else on_device
        return jax.shard_map(
            body, mesh=mesh, in_specs=placed, out_specs=P(("sp", "tp"), None), check_vma=False
        )(*args)

    return layer
```
